512 devices in a mesh: grp: 2 (over y), fs: 32 (over z), tp: 8 (over x, core).
Axes of the slice: x: 4, y: 2, z: 32, core: 2. Of those that a mesh axis runs over, the one named last changes fastest.
The devices are a block of a 4x8x32 slice.
Arguments:
- tokens: bfloat16 [12288, 2048], P(('grp', 'fs'), 'tp'), parts along dimension 0, may hold values from -40 to 40
- routes: int32 [12288, 8], P(('grp', 'fs')), parts along dimension 0, may hold values from 0 to 31, all different within a row; in each aligned block of 192 rows (0 to 191, 192 to 383, ...) at most 56 rows name the same one
- routing_weight: float32 [12288, 8], P(('grp', 'fs')), parts along dimension 0, may hold values from 0.1 to 0.6
- norm_gain_vector: float32 [2048], P('tp'), may hold values from 0.1 to 1.9
- expert_gate: float32 [32, 512, 2048], P(None, 'fs', 'tp'), may hold values from -0.125 to 0.125
- expert_up: float32 [32, 512, 2048], P(None, 'fs', 'tp'), may hold values from -0.125 to 0.125
- expert_down: float32 [32, 512, 2048], P(None, 'fs', 'tp'), may hold values from -0.25 to 0.25
- shared_gate: float32 [512, 2048], P('fs', 'tp'), may hold values from -0.125 to 0.125
- shared_up: float32 [512, 2048], P('fs', 'tp'), may hold values from -0.125 to 0.125
- shared_down: float32 [512, 2048], P('fs', 'tp'), may hold values from -0.25 to 0.25
Outputs:
- mixed: bfloat16 [12288, 2048], P(('grp', 'fs'), 'tp'), parts along dimension 0
- gate_served: bfloat16 [64, 512, 2048], P(('grp', 'fs'), None, 'tp'), parts along dimension 0
- up_served: bfloat16 [64, 512, 2048], P(('grp', 'fs'), None, 'tp'), parts along dimension 0
- down_served: bfloat16 [64, 512, 2048], P(('grp', 'fs'), None, 'tp'), parts along dimension 0
- shared_gate_served: bfloat16 [1024, 2048], P('grp', 'tp'), parts along dimension 0
- shared_up_served: bfloat16 [1024, 2048], P('grp', 'tp'), parts along dimension 0
- shared_down_served: bfloat16 [1024, 2048], P('grp', 'tp'), parts along dimension 0
The draws below stay inside these ranges and needn't reach their ends.
There are 2 independent parts, one for each index of `grp`. The reference program is written for one: setup_inputs(seed, part) draws one part's arguments, and reference() takes and returns one part's arrays. A program takes and returns all parts, laid end to end along the dimension named above; an argument that names none is the same for every part. Nothing has to cross between parts.
Inputs may be any that keep to these rules, and one draw needn't show every extreme that they name: `routes`: each row names 8 different experts. In each aligned block of 192 rows no expert is named by more than 56 rows, and in some block an expert is named by exactly 56 rows.
All inputs are finite; a program needn't handle non-finite values.
Results may differ from the reference program's by a relative error of at most 0.022.
Values may be sent and summed in bfloat16 or wider, within the bound.
A program may use at most 64 MiB of HBM per device.

```python
import math
import jax
import jax.numpy as jnp
import numpy as np
from jax import lax

D = 2048
FF = 512
SFF = 512
TOK_G = 192
EXPERTS = 32
TOPK = 8
CAP = 56
TOKENS = 6144
N_FS = 32
N_TP = 8


def draw_tokens(key, part):
    base_key = jax.random.fold_in(key, 11)
    first, second = jax.random.split(base_key, 2)
    column = jnp.arange(D).astype(jnp.float32)
    trend = 1.0 + 2.0 * column / (D - 1)
    rough = jnp.exp(jax.random.uniform(second, (D,), jnp.float32) * jnp.log(10.0))
    scales = trend * rough
    scales = scales / jnp.sqrt(jnp.mean(scales * scales))
    values = jax.random.normal(first, (TOKENS, D), jnp.float32) * scales[None, :]
    return jnp.clip(values, -40.0, 40.0).astype(jnp.bfloat16)


def shard_levels(stream_key, extent, shards, smallest, top_value):
    def one(dim, parts):
        steps = jax.random.uniform(jax.random.fold_in(jax.random.fold_in(stream_key, 6), dim), (parts,), jnp.float32, smallest / len(shards), top_value / len(shards))
        return jnp.repeat(jnp.exp(steps), extent[dim] // parts).reshape((-1,) + (1,) * (len(extent) - dim - 1))

    factor_of = one(*shards[0])
    for cut in shards[1:]:
        factor_of = factor_of * one(*cut)
    return factor_of


def deal_out(key, own, number, rows, amount, top, most, slope):
    order = jax.random.permutation(key, amount)
    packed, usual = portions_of(amount, rows * top, most, slope, True), portions_of(amount, rows * top, most, slope, False)
    places = jnp.arange(amount)

    def named(sizes, rotation):
        used = int((sizes > 0).sum())
        fixed = max(1, used // 4)
        moved = fixed + (places - fixed + rotation * (used - fixed)) % max(1, amount - fixed)
        return jnp.zeros((amount,), jnp.int32).at[order[jnp.where(places < fixed, places, moved)]].set(jnp.asarray(sizes, jnp.int32))

    sizes = jnp.where(number % 4 == 0, named(packed, number // 4), named(usual, number - number // 4 - 1))
    mixed = jax.random.permutation(jax.random.fold_in(own, 3), amount)
    giver, taker = mixed[0:amount // 2 * 2:2], mixed[1:amount // 2 * 2:2]
    margin = jnp.minimum(sizes[giver] - 1, most - sizes[taker]) // 2
    margin = jnp.where((giver == order[0]) | (taker == order[0]) | (sizes[taker] == 0), 0, jnp.maximum(margin, 0))
    moved = jax.random.randint(jax.random.fold_in(own, 4), (amount // 2,), 0, 1 << 20) % (margin + 1)
    sizes = sizes.at[giver].add(-moved).at[taker].add(moved)
    labels = jnp.searchsorted(jnp.cumsum(sizes), jnp.arange(rows * top), side="right").astype(jnp.int32)
    grid = labels.reshape(top, rows).T
    grid = grid[jax.random.permutation(jax.random.fold_in(own, 1), rows)]
    rotation = jax.random.randint(jax.random.fold_in(own, 2), (rows, 1), 0, top)
    return jnp.take_along_axis(grid, (jnp.arange(top)[None, :] + rotation) % top, axis=1)


def portions_of(count, total, most, slope, full):
    weights = [(1 << 20) // math.isqrt(standing ** slope) + 1 for standing in range(1, count + 1)]
    largest = most if full else min(most, max(-(-total // count), total * weights[0] // sum(weights)))
    least = 1 if total - largest >= count - 1 else 0
    counts, spare = [largest] + [least] * (count - 1), total - largest - least * (count - 1)
    while spare > 0:
        candidates = [i for i in range(1, count) if counts[i] < largest] or [i for i in range(1, count) if counts[i] < most]
        mass, left = sum([weights[i] for i in candidates]), spare
        for i in candidates:
            extra = min(most - counts[i], max(1, left * weights[i] // mass), spare)
            counts[i] = counts[i] + extra
            spare = spare - extra
    return np.array(counts)


def noise(key, dims, spread, reach, cuts=(), held_as=jnp.bfloat16):
    drawn = jax.random.normal(key, dims, jnp.float32) * spread
    if len(cuts) > 0:
        drawn = shard_levels(key, dims, cuts, -0.22, 0.18) * drawn
    return jnp.clip(drawn, min=-reach, max=reach).astype(held_as)


def setup_inputs(seed: int = 0, part: int = 0) -> dict:
    splits = jax.random.split(jax.random.key(seed), 11)
    part_splits = jax.random.split(jax.random.fold_in(splits[10], part), 11)
    tokens = draw_tokens(jax.random.fold_in(jax.random.fold_in(splits[10], part), 71), part)
    routes_keys = jax.random.split(jax.random.fold_in(part_splits[1], 1), TOKENS // TOK_G)
    routes_turns = jax.random.permutation(jax.random.fold_in(part_splits[1], 3), TOKENS // TOK_G)
    routes = jax.vmap(lambda own, number: deal_out(jax.random.fold_in(part_splits[1], 2), own, number, TOK_G, EXPERTS, TOPK, CAP, 1))(routes_keys, routes_turns).reshape((TOKENS, TOPK))
    routing_weight = jnp.clip(0.1 + 0.5 * jax.random.uniform(part_splits[2], (TOKENS, TOPK), jnp.float32) ** shard_levels(part_splits[2], (TOKENS, TOPK), ((0, 32),), -0.2, 0.2), 0.1, 0.6)
    norm_gain_vector = jnp.clip(1.0 + 0.18 * jax.random.normal(splits[3], (D,), jnp.float32), 0.1, 1.9)
    expert_gate = noise(splits[4], (EXPERTS, FF, D), D ** -0.5, 0.125, ((1, 32), (2, 8)), jnp.float32)
    expert_up = noise(splits[5], (EXPERTS, FF, D), D ** -0.5, 0.125, ((1, 32), (2, 8)), jnp.float32)
    expert_down = noise(splits[6], (EXPERTS, FF, D), FF ** -0.5, 0.25, ((1, 32), (2, 8)), jnp.float32)
    shared_gate = noise(splits[7], (SFF, D), D ** -0.5, 0.125, ((0, 32), (1, 8)), jnp.float32)
    shared_up = noise(splits[8], (SFF, D), D ** -0.5, 0.125, ((0, 32), (1, 8)), jnp.float32)
    shared_down = noise(splits[9], (SFF, D), SFF ** -0.5, 0.25, ((0, 32), (1, 8)), jnp.float32)
    return {"tokens": tokens, "routes": routes, "routing_weight": routing_weight, "norm_gain_vector": norm_gain_vector, "expert_gate": expert_gate, "expert_up": expert_up, "expert_down": expert_down, "shared_gate": shared_gate, "shared_up": shared_up, "shared_down": shared_down}


norm_eps = 1e-06

def block_sums(rows, weight):
    count = rows.shape[0]
    outs = weight.shape[0]
    part = D // N_TP
    left_operand = rows.astype(jnp.float32).reshape(count, N_TP, part)
    right_operand = weight.astype(jnp.float32).reshape(outs, N_TP, part)
    fragments = jnp.einsum('ucb,xcb->cux', left_operand, right_operand)
    rounded = lax.optimization_barrier(fragments.astype(jnp.bfloat16))
    return lax.optimization_barrier(jnp.sum(rounded.astype(jnp.float32), axis=0))

def reference(tokens, routes, routing_weight, norm_gain_vector, expert_gate, expert_up, expert_down, shared_gate, shared_up, shared_down):
    gate_served = (expert_gate * norm_gain_vector[None, None, :]).astype(jnp.bfloat16)
    up_served = (expert_up * norm_gain_vector[None, None, :]).astype(jnp.bfloat16)
    down_served = expert_down.astype(jnp.bfloat16)
    shared_gate_served = (shared_gate * norm_gain_vector[None, :]).astype(jnp.bfloat16)
    shared_up_served = (shared_up * norm_gain_vector[None, :]).astype(jnp.bfloat16)
    shared_down_served = shared_down.astype(jnp.bfloat16)
    values = tokens.astype(jnp.float32)
    squares = lax.optimization_barrier(jnp.sum(values * values, axis=1, keepdims=True))
    normed = (values * lax.rsqrt(squares / D + norm_eps)).astype(jnp.bfloat16)
    grouped = routes.reshape(N_FS, TOK_G * TOPK)
    onehot = (grouped[:, :, None] == jnp.arange(EXPERTS, dtype=jnp.int32)[None, None, :]).astype(jnp.int32)
    earlier = jnp.cumsum(onehot, axis=1) - onehot
    slot_index = lax.optimization_barrier(jnp.sum(earlier * onehot, axis=2))
    blocks = jnp.arange(N_FS, dtype=jnp.int32)[:, None]
    target = (grouped * (N_FS * CAP) + blocks * CAP + slot_index).reshape(-1).astype(jnp.int32)
    token_ids = jnp.repeat(jnp.arange(TOKENS, dtype=jnp.int32), TOPK)
    row_table = jnp.full((EXPERTS * N_FS * CAP,), TOKENS, jnp.int32).at[target].set(token_ids)
    row_table = row_table.reshape(EXPERTS, N_FS * CAP)
    weight_table = jnp.zeros((EXPERTS * N_FS * CAP,), jnp.float32).at[target].set(routing_weight.reshape(-1).astype(jnp.float32))
    weight_table = weight_table.reshape(EXPERTS, N_FS * CAP)
    padded = jnp.concatenate([normed, jnp.zeros((1, D), jnp.bfloat16)], axis=0)

    def one_expert(total, items):
        row_ids, weights, gate_w, up_w, down_w = items
        rows = padded[row_ids]
        hidden = (jax.nn.silu(block_sums(rows, gate_w)) * block_sums(rows, up_w)).astype(jnp.bfloat16)
        produced = jnp.dot(hidden, down_w, preferred_element_type=jnp.float32).astype(jnp.bfloat16)
        return (total.at[row_ids].add(weights[:, None] * produced.astype(jnp.float32)), None)
    routed, _ = lax.scan(one_expert, jnp.zeros((TOKENS + 1, D), jnp.float32), (row_table, weight_table, gate_served, up_served, down_served))
    shared_hidden = (jax.nn.silu(block_sums(normed, shared_gate_served)) * block_sums(normed, shared_up_served)).astype(jnp.bfloat16)
    shared_out = jnp.dot(shared_hidden, shared_down_served, preferred_element_type=jnp.float32)
    mixed = (routed[:TOKENS] + shared_out).astype(jnp.bfloat16)
    return (mixed, gate_served, up_served, down_served, shared_gate_served, shared_up_served, shared_down_served)
```

```python
import functools

import jax
import jax.numpy as jnp
from jax import lax
from jax.experimental import pallas as pl
from jax.experimental.pallas import tpu as pltpu
from jax.sharding import PartitionSpec as P

norm_eps = 1e-06
MESH = pl.DeviceIdType.MESH
GATHER_PIECES = 4
REDUCE_PIECES = 4
BF16 = jnp.bfloat16
F32 = jnp.float32


def contract(a, b, da, db):
    return lax.dot_general(a, b, (((da,), (db,)), ((), ())), preferred_element_type=F32)


def barrier_with(peers):
    barrier = pltpu.get_barrier_semaphore()
    for peer in peers:
        pl.semaphore_signal(barrier, inc=1, device_id=peer, device_id_type=MESH)
    pl.semaphore_wait(barrier, len(peers))


def gather_kernel(n, pieces, block, out, send_sem, recv_sem, own_sem):
    me = lax.axis_index("fs")
    right, left = lax.rem(me + 1, n), lax.rem(me + n - 1, n)
    rows = block.shape[0] // pieces
    reach = (n // 2, n - 1 - n // 2)

    def copy(way, step, piece, first=False):
        whose = lax.rem(me + n - step, n) if way == 0 else lax.rem(me + step, n)
        part = pl.ds(piece * rows, rows)
        target = out.at[whose, part, :]
        return pltpu.make_async_remote_copy(
            src_ref=block.at[part, :] if first else target,
            dst_ref=target,
            send_sem=send_sem.at[way, step, piece],
            recv_sem=recv_sem.at[way, step, piece],
            device_id={"fs": right if way == 0 else left},
            device_id_type=MESH,
        )

    def arrived(way, step, piece):
        whose = lax.rem(me + 2 * n - step - 1, n) if way == 0 else lax.rem(me + step + 1, n)
        target = out.at[whose, pl.ds(piece * rows, rows), :]
        pltpu.make_async_remote_copy(
            src_ref=target,
            dst_ref=target,
            send_sem=send_sem.at[way, step, piece],
            recv_sem=recv_sem.at[way, step, piece],
            device_id={"fs": left if way == 0 else right},
            device_id_type=MESH,
        ).wait_recv()

    own = pltpu.make_async_copy(block, out.at[me], own_sem)
    own.start()
    barrier_with([{"fs": left}, {"fs": right}])
    for piece in range(pieces):
        for way in range(2):
            if reach[way] > 0:
                copy(way, 0, piece, True).start()

    def step_of(ways):
        def body(step, carry):
            for piece in range(pieces):
                for way in ways:
                    arrived(way, step - 1, piece)
                    copy(way, step, piece).start()
            return carry

        return body

    lax.fori_loop(1, reach[1], step_of((0, 1)), 0)
    lax.fori_loop(max(reach[1], 1), reach[0], step_of((0,)), 0)
    for piece in range(pieces):
        for way in range(2):
            if reach[way] > 0:
                arrived(way, reach[way] - 1, piece)
    own.wait()
    for way in range(2):
        for piece in range(pieces):
            copy(way, 0, piece, True).wait_send()

        def sent(step, carry, way=way):
            for piece in range(pieces):
                copy(way, step, piece).wait_send()
            return carry

        lax.fori_loop(1, reach[way], sent, 0)


def ring_gather(n, block):
    reach = n // 2
    return pl.pallas_call(
        functools.partial(gather_kernel, n, GATHER_PIECES),
        out_shape=jax.ShapeDtypeStruct((n,) + block.shape, block.dtype),
        in_specs=[pl.BlockSpec(memory_space=pltpu.VMEM)],
        out_specs=pl.BlockSpec(memory_space=pltpu.VMEM),
        scratch_shapes=[
            pltpu.SemaphoreType.DMA((2, reach, GATHER_PIECES)),
            pltpu.SemaphoreType.DMA((2, reach, GATHER_PIECES)),
            pltpu.SemaphoreType.DMA,
        ],
        compiler_params=pltpu.CompilerParams(collective_id=0, has_side_effects=True),
        cost_estimate=pl.CostEstimate(flops=10**9, bytes_accessed=10**7, transcendentals=0),
        name="ring_gather",
    )(block)


def layer_kernel(
    n,
    tp,
    shared_rows,
    pieces,
    rows_ref,
    gate_ref,
    up_ref,
    down_ref,
    sgate_ref,
    sup_ref,
    sdown_ref,
    place_ref,
    out_ref,
    psend,
    precv,
    total,
    passed,
    direct,
    final,
    own_total,
    hidden,
    combined,
    shared_out,
    ring,
    pair_send,
    pair_recv,
    sum_send,
    sum_recv,
    hid_send,
    hid_recv,
    ring_send,
    ring_recv,
):
    me = lax.axis_index("fs")
    t = lax.axis_index("tp")
    right, left = lax.rem(me + 1, n), lax.rem(me + n - 1, n)
    chips = tp // 2
    x, core = t // 2, lax.rem(t, 2)

    def chip(offset):
        return lax.rem(x + offset + chips, chips)

    mate = 2 * x + 1 - core
    ahead, behind = 2 * chip(1) + core, 2 * chip(-1) + core
    share_rows, width = rows_ref.shape[1], 2 * gate_ref.shape[0]
    ff = gate_ref.shape[0]
    routed = share_rows - (share_rows - n // tp * place_ref.shape[1])
    half = share_rows // 2

    barrier_with(
        [{"fs": left}, {"fs": right}, {"tp": mate}, {"tp": ahead}, {"tp": behind}]
    )

    def partial_sums(share, put):
        put(0, routed, 0, contract(rows_ref[share, 0:routed, :], gate_ref[...], 1, 1))
        put(0, routed, ff, contract(rows_ref[share, 0:routed, :], up_ref[...], 1, 1))
        put(routed, share_rows, 0, contract(rows_ref[share, routed:, :], sgate_ref[...], 1, 1))
        put(routed, share_rows, ff, contract(rows_ref[share, routed:, :], sup_ref[...], 1, 1))

    def remote(src, dst, send_sem, recv_sem, peer):
        return pltpu.make_async_remote_copy(
            src_ref=src,
            dst_ref=dst,
            send_sem=send_sem,
            recv_sem=recv_sem,
            device_id={"tp": peer},
            device_id_type=MESH,
        )

    def pair_copy(r):
        return remote(psend.at[r], precv.at[r], pair_send.at[r], pair_recv.at[r], mate)

    for r in (2, 1, 3, 0):

        def put(a, b, c, value, r=r):
            psend[r, a:b, c : c + ff] = value.astype(BF16)

        partial_sums(2 * chip(r) + 1 - core, put)
        pair_copy(r).start()

    top, low = pl.ds(0, half), pl.ds(half, half)
    pass_top = remote(total.at[2, top, :], passed.at[0], sum_send.at[0], sum_recv.at[0], ahead)
    pass_low = remote(total.at[2, low, :], passed.at[1], sum_send.at[1], sum_recv.at[1], behind)
    direct_low = remote(total.at[1, low, :], direct.at[1], sum_send.at[2], sum_recv.at[2], ahead)
    direct_top = remote(total.at[3, top, :], direct.at[0], sum_send.at[3], sum_recv.at[3], behind)
    final_top = remote(total.at[1, top, :], final.at[0], sum_send.at[4], sum_recv.at[4], ahead)
    final_low = remote(total.at[3, low, :], final.at[1], sum_send.at[5], sum_recv.at[5], behind)
    for r in (2, 1, 3, 0):
        pair_copy(r).wait_recv()

        def put(a, b, c, value, r=r):
            value = value + precv[r, a:b, c : c + ff].astype(F32)
            if r == 0:
                own_total[a:b, c : c + ff] = value
            else:
                total[r, a:b, c : c + ff] = value.astype(BF16)

        partial_sums(2 * chip(r) + core, put)
        if r == 2:
            pass_top.start()
            pass_low.start()
        if r == 1:
            direct_low.start()
        if r == 3:
            direct_top.start()

    def add_rows(slot, start, source):
        total[slot, start : start + half, :] = (
            total[slot, start : start + half, :].astype(F32) + source.astype(F32)
        ).astype(BF16)

    pass_top.wait_recv()
    add_rows(1, 0, passed[0])
    final_top.start()
    pass_low.wait_recv()
    add_rows(3, half, passed[1])
    final_low.start()
    direct_low.wait_recv()
    direct_top.wait_recv()
    final_top.wait_recv()
    final_low.wait_recv()

    for k in range(2):
        span = slice(k * half, (k + 1) * half)

        def summed(c, k=k, span=span):
            cols = slice(c, c + ff)
            return (
                own_total[span, cols]
                + direct[k, :, cols].astype(F32)
                + final[k, :, cols].astype(F32)
            )

        g = summed(0)
        hidden[t, span, :] = (g / (1.0 + jnp.exp(-g)) * summed(ff)).astype(BF16)

    def hid(slot, span, k, peer):
        ref = hidden.at[slot, span, :]
        return remote(ref, ref, hid_send.at[k], hid_recv.at[k], peer)

    whole = pl.ds(0, share_rows)
    mine, opposite = t, 2 * chip(2) + core
    hid(mine, whole, 1, ahead).start()
    hid(mine, whole, 2, behind).start()
    hid(mine, whole, 0, mate).start()
    hid(behind, whole, 1, behind).wait_recv()
    hid(behind, top, 3, ahead).start()
    hid(behind, whole, 5, mate).start()
    hid(ahead, whole, 2, ahead).wait_recv()
    hid(ahead, low, 4, behind).start()
    hid(ahead, whole, 6, mate).start()
    hid(opposite, top, 3, behind).wait_recv()
    hid(opposite, top, 7, mate).start()
    hid(opposite, low, 4, ahead).wait_recv()
    hid(opposite, low, 8, mate).start()

    def other(slot):
        return 2 * (slot // 2) + 1 - lax.rem(slot, 2)

    hid(other(mine), whole, 0, mate).wait_recv()
    hid(other(behind), whole, 5, mate).wait_recv()
    hid(other(ahead), whole, 6, mate).wait_recv()
    hid(other(opposite), top, 7, mate).wait_recv()
    hid(other(opposite), low, 8, mate).wait_recv()

    per_share = n // tp
    capacity = place_ref.shape[1]

    def down_of(share, carry):
        produced = contract(hidden[share, 0:routed, :], down_ref[...], 1, 0)
        for q in range(per_share):
            piece = produced[q * capacity : (q + 1) * capacity, :].astype(BF16)
            block = share * per_share + q
            combined[block] = contract(place_ref[block], piece, 0, 0).astype(BF16)
        extra = contract(hidden[share, routed:, :], sdown_ref[...], 1, 0)
        start = pl.multiple_of(share * shared_rows, 8)
        shared_out[pl.ds(start, shared_rows), :] = extra[0:shared_rows, :]
        return carry

    lax.fori_loop(0, tp, down_of, 0)

    reach = (n // 2, n - 1 - n // 2)
    size = combined.shape[1] // pieces

    def spot(way, step):
        ahead_by = reach[way] - step
        return lax.rem(me + ahead_by, n) if way == 0 else lax.rem(me + n - ahead_by, n)

    def ring_copy(way, step, piece, first=False):
        part = pl.ds(piece * size, size)
        if first:
            src = combined.at[spot(way, step), part, :]
        else:
            src = ring.at[way, step - 1, part, :]
        return pltpu.make_async_remote_copy(
            src_ref=src,
            dst_ref=ring.at[way, step, part, :],
            send_sem=ring_send.at[way, step, piece],
            recv_sem=ring_recv.at[way, step, piece],
            device_id={"fs": right if way == 0 else left},
            device_id_type=MESH,
        )

    for piece in range(pieces):
        for way in range(2):
            ring_copy(way, 0, piece, True).start()

    def ring_step(ways):
        def body(step, carry):
            for piece in range(pieces):
                for way in ways:
                    ring_copy(way, step - 1, piece, True).wait_recv()
                    part = pl.ds(piece * size, size)
                    ring[way, step - 1, part, :] = (
                        ring[way, step - 1, part, :].astype(F32)
                        + combined[spot(way, step), part, :].astype(F32)
                    ).astype(BF16)
                    ring_copy(way, step, piece).start()
            return carry

        return body

    lax.fori_loop(1, reach[1], ring_step((0, 1)), 0)
    lax.fori_loop(max(reach[1], 1), reach[0], ring_step((0,)), 0)
    for piece in range(pieces):
        part = slice(piece * size, (piece + 1) * size)
        for way in range(2):
            ring_copy(way, reach[way] - 1, piece, True).wait_recv()
        out_ref[part, :] = (
            ring[0, reach[0] - 1, part, :].astype(F32)
            + ring[1, reach[1] - 1, part, :].astype(F32)
            + combined[me, part, :].astype(F32)
            + shared_out[part, :]
        ).astype(BF16)

    for r in range(4):
        pair_copy(r).wait_send()
    for c in (pass_top, pass_low, direct_low, direct_top, final_top, final_low):
        c.wait_send()
    for span, ks in ((whole, (0, 1, 2, 5, 6)), (top, (3, 7)), (low, (4, 8))):
        for k in ks:
            hid(mine, span, k, mate).wait_send()
    for way in range(2):
        for piece in range(pieces):
            ring_copy(way, 0, piece, True).wait_send()

        def sent(step, carry, way=way):
            for piece in range(pieces):
                ring_copy(way, step, piece).wait_send()
            return carry

        lax.fori_loop(1, reach[way], sent, 0)


def run_layer(n, tp, tok_rows, rows, weights, place):
    shares, share_rows, width = rows.shape
    ff = weights[0].shape[0]
    chips, half = tp // 2, share_rows // 2
    reach = n // 2
    dma = pltpu.SemaphoreType.DMA
    return pl.pallas_call(
        functools.partial(layer_kernel, n, tp, tok_rows // tp, REDUCE_PIECES),
        out_shape=jax.ShapeDtypeStruct((tok_rows, width), BF16),
        in_specs=[pl.BlockSpec(memory_space=pltpu.VMEM)] * 8,
        out_specs=pl.BlockSpec(memory_space=pltpu.VMEM),
        scratch_shapes=[
            pltpu.VMEM((chips, share_rows, 2 * ff), BF16),
            pltpu.VMEM((chips, share_rows, 2 * ff), BF16),
            pltpu.VMEM((chips, share_rows, 2 * ff), BF16),
            pltpu.VMEM((2, half, 2 * ff), BF16),
            pltpu.VMEM((2, half, 2 * ff), BF16),
            pltpu.VMEM((2, half, 2 * ff), BF16),
            pltpu.VMEM((share_rows, 2 * ff), F32),
            pltpu.VMEM((tp, share_rows, ff), BF16),
            pltpu.VMEM((n, tok_rows, width), BF16),
            pltpu.VMEM((tok_rows, width), F32),
            pltpu.VMEM((2, reach, tok_rows, width), BF16),
            dma((chips,)),
            dma((chips,)),
            dma((6,)),
            dma((6,)),
            dma((9,)),
            dma((9,)),
            dma((2, reach, REDUCE_PIECES)),
            dma((2, reach, REDUCE_PIECES)),
        ],
        compiler_params=pltpu.CompilerParams(collective_id=1, has_side_effects=True),
        cost_estimate=pl.CostEstimate(flops=2 * 10**9, bytes_accessed=10**7, transcendentals=0),
        name="expert_layer",
    )(rows, *weights, place)


def per_device(
    n,
    tp,
    tokens,
    routes,
    routing_weight,
    norm_gain_vector,
    expert_gate,
    expert_up,
    expert_down,
    shared_gate,
    shared_up,
    shared_down,
):
    tok_rows, width = tokens.shape
    experts = expert_gate.shape[0]
    top_count = routes.shape[1]
    capacity = tok_rows * top_count * 7 // (6 * experts)
    gain = norm_gain_vector
    both = jnp.concatenate(
        [
            (expert_gate * gain[None, None, :]).astype(BF16),
            (expert_up * gain[None, None, :]).astype(BF16),
            expert_down.astype(BF16),
        ],
        axis=2,
    )
    moved = lax.all_to_all(both, "fs", split_axis=0, concat_axis=1, tiled=True)
    gate_new, up_new, down_new = jnp.split(moved, 3, axis=2)

    values = tokens.astype(F32)
    totals = lax.psum(jnp.sum(values * values, axis=1), "tp")
    normed = (values * lax.rsqrt(totals / (width * tp) + norm_eps)[:, None]).astype(BF16)

    def as_lanes(a):
        return jnp.pad(a.T.astype(BF16), ((0, 0), (0, width - tok_rows)))

    block = jnp.concatenate(
        [
            normed,
            (shared_gate * gain[None, :]).astype(BF16),
            (shared_up * gain[None, :]).astype(BF16),
            shared_down.astype(BF16),
            as_lanes(routes),
            as_lanes(routing_weight),
        ],
        axis=0,
    )
    got = ring_gather(n, block)
    unit = shared_gate.shape[0]
    at = tok_rows
    shared = []
    for _ in range(3):
        shared.append(got[:, at : at + unit, :].reshape(n * unit, width))
        at += unit
    sgate, sup, sdown = shared
    chosen_by = got[:, at : at + top_count, :tok_rows]
    weight_of = got[:, at + top_count : at + 2 * top_count, :tok_rows]
    mine = chosen_by.astype(F32) == lax.axis_index("fs").astype(F32)
    weights = jnp.sum(jnp.where(mine, weight_of.astype(F32), 0.0), axis=1)
    named = jnp.any(mine, axis=1)
    index = jnp.arange(tok_rows, dtype=jnp.int32)
    before = (index[:, None] < index[None, :]).astype(BF16)
    rank = jnp.dot(named.astype(BF16), before, preferred_element_type=F32)
    slot = jnp.where(named, rank, -1.0)
    hit = slot[:, None, :] == jnp.arange(capacity, dtype=jnp.int32).astype(F32)[None, :, None]
    place = jnp.where(hit, weights[:, None, :], 0.0).astype(BF16)
    picked = jnp.einsum(
        "bsj,bjd->bsd", hit.astype(BF16), got[:, :tok_rows, :], preferred_element_type=F32
    ).astype(BF16)
    per_share = n // tp * capacity
    shared_rows = tok_rows // tp
    rows = jnp.concatenate(
        [
            picked.reshape(tp, per_share, width),
            normed.reshape(tp, shared_rows, width),
            jnp.zeros((tp, -(per_share + shared_rows) % 32, width), BF16),
        ],
        axis=1,
    )
    mixed = run_layer(
        n,
        tp,
        tok_rows,
        rows,
        (gate_new[0], up_new[0], down_new[0], sgate, sup, sdown),
        place,
    )
    return (mixed, gate_new, up_new, down_new, sgate, sup, sdown)


def solution(mesh):
    return jax.shard_map(
        functools.partial(per_device, mesh.shape["fs"], mesh.shape["tp"]),
        mesh=mesh,
        in_specs=(
            P(("grp", "fs"), "tp"),
            P(("grp", "fs"), None),
            P(("grp", "fs"), None),
            P("tp"),
            P(None, "fs", "tp"),
            P(None, "fs", "tp"),
            P(None, "fs", "tp"),
            P("fs", "tp"),
            P("fs", "tp"),
            P("fs", "tp"),
        ),
        out_specs=(
            P(("grp", "fs"), "tp"),
            P(("grp", "fs"), None, "tp"),
            P(("grp", "fs"), None, "tp"),
            P(("grp", "fs"), None, "tp"),
            P("grp", "tp"),
            P("grp", "tp"),
            P("grp", "tp"),
        ),
        check_vma=False,
    )
```

```python
import functools

import jax
import jax.numpy as jnp
from jax import lax
from jax.experimental import pallas as pl
from jax.experimental.pallas import tpu as pltpu
from jax.sharding import PartitionSpec as P

norm_eps = 1e-06
MESH = pl.DeviceIdType.MESH
GATHER_PIECES = 4
REDUCE_PIECES = 4
BF16 = jnp.bfloat16
F32 = jnp.float32


def contract(a, b, da, db):
    return lax.dot_general(a, b, (((da,), (db,)), ((), ())), preferred_element_type=F32)


def barrier_with(peers):
    barrier = pltpu.get_barrier_semaphore()
    for peer in peers:
        pl.semaphore_signal(barrier, inc=1, device_id=peer, device_id_type=MESH)
    pl.semaphore_wait(barrier, len(peers))


def gather_kernel(
    n, groups, pieces, block, held, out, full, send_sem, recv_sem, own_sem, y_send, y_recv, y_own
):
    me = lax.axis_index("fs")
    group = lax.axis_index("grp")
    cols, share = full.shape[0], held.shape[1]
    right, left = lax.rem(me + 1, n), lax.rem(me + n - 1, n)
    rows = block.shape[0] // pieces
    reach = (n // 2, n - 1 - n // 2)

    def copy(way, step, piece, first=False):
        whose = lax.rem(me + n - step, n) if way == 0 else lax.rem(me + step, n)
        part = pl.ds(piece * rows, rows)
        target = out.at[whose, part, :]
        return pltpu.make_async_remote_copy(
            src_ref=block.at[part, :] if first else target,
            dst_ref=target,
            send_sem=send_sem.at[way, step, piece],
            recv_sem=recv_sem.at[way, step, piece],
            device_id={"fs": right if way == 0 else left},
            device_id_type=MESH,
        )

    def arrived(way, step, piece):
        whose = lax.rem(me + 2 * n - step - 1, n) if way == 0 else lax.rem(me + step + 1, n)
        target = out.at[whose, pl.ds(piece * rows, rows), :]
        pltpu.make_async_remote_copy(
            src_ref=target,
            dst_ref=target,
            send_sem=send_sem.at[way, step, piece],
            recv_sem=recv_sem.at[way, step, piece],
            device_id={"fs": left if way == 0 else right},
            device_id_type=MESH,
        ).wait_recv()

    own = pltpu.make_async_copy(block, out.at[me], own_sem)
    own.start()
    others = [lax.rem(group + j, groups) for j in range(1, groups)]
    barrier_with([{"fs": left}, {"fs": right}] + [{"grp": g} for g in others])
    for piece in range(pieces):
        for way in range(2):
            if reach[way] > 0:
                copy(way, 0, piece, True).start()

    def handed(j, i, sender):
        piece = sender * share + i
        peer = lax.rem(group + j, groups)
        return piece < cols, lambda: pltpu.make_async_remote_copy(
            src_ref=held.at[:, i],
            dst_ref=full.at[jnp.minimum(piece, cols - 1)],
            send_sem=y_send.at[j - 1, i],
            recv_sem=y_recv.at[j - 1, i],
            device_id={"grp": peer},
            device_id_type=MESH,
        )

    def kept(i):
        piece = group * share + i
        return piece < cols, lambda: pltpu.make_async_copy(
            held.at[:, i], full.at[jnp.minimum(piece, cols - 1)], y_own.at[i]
        )

    def when_all(pairs, act):
        for used, make in pairs:

            @pl.when(used)
            def _(make=make):
                act(make())

    order = [(j, i) for j in range(1, groups) for i in range(share)]
    when_all([handed(j, i, group) for j, i in order], lambda c: c.start())
    when_all([kept(i) for i in range(share)], lambda c: c.start())

    def step_of(ways):
        def body(step, carry):
            for piece in range(pieces):
                for way in ways:
                    arrived(way, step - 1, piece)
                    copy(way, step, piece).start()
            return carry

        return body

    lax.fori_loop(1, reach[1], step_of((0, 1)), 0)
    lax.fori_loop(max(reach[1], 1), reach[0], step_of((0,)), 0)
    for piece in range(pieces):
        for way in range(2):
            if reach[way] > 0:
                arrived(way, reach[way] - 1, piece)
    own.wait()
    senders = [(j, i, lax.rem(group + groups - j, groups)) for j, i in order]
    when_all([handed(j, i, sender) for j, i, sender in senders], lambda c: c.wait_recv())
    when_all([kept(i) for i in range(share)], lambda c: c.wait())
    when_all([handed(j, i, group) for j, i in order], lambda c: c.wait_send())
    for way in range(2):
        for piece in range(pieces):
            copy(way, 0, piece, True).wait_send()

        def sent(step, carry, way=way):
            for piece in range(pieces):
                copy(way, step, piece).wait_send()
            return carry

        lax.fori_loop(1, reach[way], sent, 0)


def ring_gather(n, groups, cols, block, held):
    reach = n // 2
    share = held.shape[1]
    vmem = pl.BlockSpec(memory_space=pltpu.VMEM)
    return pl.pallas_call(
        functools.partial(gather_kernel, n, groups, GATHER_PIECES),
        out_shape=(
            jax.ShapeDtypeStruct((n,) + block.shape, block.dtype),
            jax.ShapeDtypeStruct((cols, n) + held.shape[2:], held.dtype),
        ),
        in_specs=[vmem, vmem],
        out_specs=(vmem, vmem),
        scratch_shapes=[
            pltpu.SemaphoreType.DMA((2, reach, GATHER_PIECES)),
            pltpu.SemaphoreType.DMA((2, reach, GATHER_PIECES)),
            pltpu.SemaphoreType.DMA,
            pltpu.SemaphoreType.DMA((max(groups - 1, 1), share)),
            pltpu.SemaphoreType.DMA((max(groups - 1, 1), share)),
            pltpu.SemaphoreType.DMA((share,)),
        ],
        compiler_params=pltpu.CompilerParams(collective_id=0, has_side_effects=True),
        cost_estimate=pl.CostEstimate(flops=10**9, bytes_accessed=10**7, transcendentals=0),
        name="ring_gather",
    )(block, held)


def layer_kernel(
    n,
    tp,
    shared_rows,
    pieces,
    rows_ref,
    gate_ref,
    up_ref,
    down_ref,
    sgate_ref,
    sup_ref,
    sdown_ref,
    place_ref,
    out_ref,
    psend,
    precv,
    total,
    passed,
    direct,
    final,
    own_total,
    hidden,
    combined,
    shared_out,
    ring,
    pair_send,
    pair_recv,
    sum_send,
    sum_recv,
    hid_send,
    hid_recv,
    ring_send,
    ring_recv,
):
    me = lax.axis_index("fs")
    t = lax.axis_index("tp")
    right, left = lax.rem(me + 1, n), lax.rem(me + n - 1, n)
    chips = tp // 2
    x, core = t // 2, lax.rem(t, 2)

    def chip(offset):
        return lax.rem(x + offset + chips, chips)

    mate = 2 * x + 1 - core
    ahead, behind = 2 * chip(1) + core, 2 * chip(-1) + core
    share_rows, width = rows_ref.shape[1], 2 * gate_ref.shape[0]
    ff = gate_ref.shape[0]
    routed = share_rows - (share_rows - n // tp * place_ref.shape[1])
    half = share_rows // 2

    barrier_with(
        [{"fs": left}, {"fs": right}, {"tp": mate}, {"tp": ahead}, {"tp": behind}]
    )

    def partial_sums(share, put):
        put(0, routed, 0, contract(rows_ref[share, 0:routed, :], gate_ref[...], 1, 1))
        put(0, routed, ff, contract(rows_ref[share, 0:routed, :], up_ref[...], 1, 1))
        put(routed, share_rows, 0, contract(rows_ref[share, routed:, :], sgate_ref[...], 1, 1))
        put(routed, share_rows, ff, contract(rows_ref[share, routed:, :], sup_ref[...], 1, 1))

    def remote(src, dst, send_sem, recv_sem, peer):
        return pltpu.make_async_remote_copy(
            src_ref=src,
            dst_ref=dst,
            send_sem=send_sem,
            recv_sem=recv_sem,
            device_id={"tp": peer},
            device_id_type=MESH,
        )

    def pair_copy(r):
        return remote(psend.at[r], precv.at[r], pair_send.at[r], pair_recv.at[r], mate)

    for r in (2, 1, 3, 0):

        def put(a, b, c, value, r=r):
            psend[r, a:b, c : c + ff] = value.astype(BF16)

        partial_sums(2 * chip(r) + 1 - core, put)
        pair_copy(r).start()

    top, low = pl.ds(0, half), pl.ds(half, half)
    pass_top = remote(total.at[2, top, :], passed.at[0], sum_send.at[0], sum_recv.at[0], ahead)
    pass_low = remote(total.at[2, low, :], passed.at[1], sum_send.at[1], sum_recv.at[1], behind)
    direct_low = remote(total.at[1, low, :], direct.at[1], sum_send.at[2], sum_recv.at[2], ahead)
    direct_top = remote(total.at[3, top, :], direct.at[0], sum_send.at[3], sum_recv.at[3], behind)
    final_top = remote(total.at[1, top, :], final.at[0], sum_send.at[4], sum_recv.at[4], ahead)
    final_low = remote(total.at[3, low, :], final.at[1], sum_send.at[5], sum_recv.at[5], behind)
    for r in (2, 1, 3, 0):
        pair_copy(r).wait_recv()

        def put(a, b, c, value, r=r):
            value = value + precv[r, a:b, c : c + ff].astype(F32)
            if r == 0:
                own_total[a:b, c : c + ff] = value
            else:
                total[r, a:b, c : c + ff] = value.astype(BF16)

        partial_sums(2 * chip(r) + core, put)
        if r == 2:
            pass_top.start()
            pass_low.start()
        if r == 1:
            direct_low.start()
        if r == 3:
            direct_top.start()

    def add_rows(slot, start, source):
        total[slot, start : start + half, :] = (
            total[slot, start : start + half, :].astype(F32) + source.astype(F32)
        ).astype(BF16)

    pass_top.wait_recv()
    add_rows(1, 0, passed[0])
    final_top.start()
    pass_low.wait_recv()
    add_rows(3, half, passed[1])
    final_low.start()
    direct_low.wait_recv()
    direct_top.wait_recv()
    final_top.wait_recv()
    final_low.wait_recv()

    for k in range(2):
        span = slice(k * half, (k + 1) * half)

        def summed(c, k=k, span=span):
            cols = slice(c, c + ff)
            return (
                own_total[span, cols]
                + direct[k, :, cols].astype(F32)
                + final[k, :, cols].astype(F32)
            )

        g = summed(0)
        hidden[t, span, :] = (g / (1.0 + jnp.exp(-g)) * summed(ff)).astype(BF16)

    def hid(slot, span, k, peer):
        ref = hidden.at[slot, span, :]
        return remote(ref, ref, hid_send.at[k], hid_recv.at[k], peer)

    whole = pl.ds(0, share_rows)
    mine, opposite = t, 2 * chip(2) + core
    hid(mine, whole, 1, ahead).start()
    hid(mine, whole, 2, behind).start()
    hid(mine, whole, 0, mate).start()
    hid(behind, whole, 1, behind).wait_recv()
    hid(behind, top, 3, ahead).start()
    hid(behind, whole, 5, mate).start()
    hid(ahead, whole, 2, ahead).wait_recv()
    hid(ahead, low, 4, behind).start()
    hid(ahead, whole, 6, mate).start()
    hid(opposite, top, 3, behind).wait_recv()
    hid(opposite, top, 7, mate).start()
    hid(opposite, low, 4, ahead).wait_recv()
    hid(opposite, low, 8, mate).start()

    def other(slot):
        return 2 * (slot // 2) + 1 - lax.rem(slot, 2)

    hid(other(mine), whole, 0, mate).wait_recv()
    hid(other(behind), whole, 5, mate).wait_recv()
    hid(other(ahead), whole, 6, mate).wait_recv()
    hid(other(opposite), top, 7, mate).wait_recv()
    hid(other(opposite), low, 8, mate).wait_recv()

    per_share = n // tp
    capacity = place_ref.shape[1]

    def down_of(share, carry):
        produced = contract(hidden[share, 0:routed, :], down_ref[...], 1, 0)
        for q in range(per_share):
            piece = produced[q * capacity : (q + 1) * capacity, :].astype(BF16)
            block = share * per_share + q
            combined[block] = contract(place_ref[block], piece, 0, 0).astype(BF16)
        extra = contract(hidden[share, routed:, :], sdown_ref[...], 1, 0)
        start = pl.multiple_of(share * shared_rows, 8)
        shared_out[pl.ds(start, shared_rows), :] = extra[0:shared_rows, :]
        return carry

    lax.fori_loop(0, tp, down_of, 0)

    reach = (n // 2, n - 1 - n // 2)
    size = combined.shape[1] // pieces

    def spot(way, step):
        ahead_by = reach[way] - step
        return lax.rem(me + ahead_by, n) if way == 0 else lax.rem(me + n - ahead_by, n)

    def ring_copy(way, step, piece, first=False):
        part = pl.ds(piece * size, size)
        if first:
            src = combined.at[spot(way, step), part, :]
        else:
            src = ring.at[way, step - 1, part, :]
        return pltpu.make_async_remote_copy(
            src_ref=src,
            dst_ref=ring.at[way, step, part, :],
            send_sem=ring_send.at[way, step, piece],
            recv_sem=ring_recv.at[way, step, piece],
            device_id={"fs": right if way == 0 else left},
            device_id_type=MESH,
        )

    for piece in range(pieces):
        for way in range(2):
            ring_copy(way, 0, piece, True).start()

    def ring_step(ways):
        def body(step, carry):
            for piece in range(pieces):
                for way in ways:
                    ring_copy(way, step - 1, piece, True).wait_recv()
                    part = pl.ds(piece * size, size)
                    ring[way, step - 1, part, :] = (
                        ring[way, step - 1, part, :].astype(F32)
                        + combined[spot(way, step), part, :].astype(F32)
                    ).astype(BF16)
                    ring_copy(way, step, piece).start()
            return carry

        return body

    lax.fori_loop(1, reach[1], ring_step((0, 1)), 0)
    lax.fori_loop(max(reach[1], 1), reach[0], ring_step((0,)), 0)
    for piece in range(pieces):
        part = slice(piece * size, (piece + 1) * size)
        for way in range(2):
            ring_copy(way, reach[way] - 1, piece, True).wait_recv()
        out_ref[part, :] = (
            ring[0, reach[0] - 1, part, :].astype(F32)
            + ring[1, reach[1] - 1, part, :].astype(F32)
            + combined[me, part, :].astype(F32)
            + shared_out[part, :]
        ).astype(BF16)

    for r in range(4):
        pair_copy(r).wait_send()
    for c in (pass_top, pass_low, direct_low, direct_top, final_top, final_low):
        c.wait_send()
    for span, ks in ((whole, (0, 1, 2, 5, 6)), (top, (3, 7)), (low, (4, 8))):
        for k in ks:
            hid(mine, span, k, mate).wait_send()
    for way in range(2):
        for piece in range(pieces):
            ring_copy(way, 0, piece, True).wait_send()

        def sent(step, carry, way=way):
            for piece in range(pieces):
                ring_copy(way, step, piece).wait_send()
            return carry

        lax.fori_loop(1, reach[way], sent, 0)


def run_layer(n, tp, tok_rows, rows, weights, place):
    shares, share_rows, width = rows.shape
    ff = weights[0].shape[0]
    chips, half = tp // 2, share_rows // 2
    reach = n // 2
    dma = pltpu.SemaphoreType.DMA
    return pl.pallas_call(
        functools.partial(layer_kernel, n, tp, tok_rows // tp, REDUCE_PIECES),
        out_shape=jax.ShapeDtypeStruct((tok_rows, width), BF16),
        in_specs=[pl.BlockSpec(memory_space=pltpu.VMEM)] * 8,
        out_specs=pl.BlockSpec(memory_space=pltpu.VMEM),
        scratch_shapes=[
            pltpu.VMEM((chips, share_rows, 2 * ff), BF16),
            pltpu.VMEM((chips, share_rows, 2 * ff), BF16),
            pltpu.VMEM((chips, share_rows, 2 * ff), BF16),
            pltpu.VMEM((2, half, 2 * ff), BF16),
            pltpu.VMEM((2, half, 2 * ff), BF16),
            pltpu.VMEM((2, half, 2 * ff), BF16),
            pltpu.VMEM((share_rows, 2 * ff), F32),
            pltpu.VMEM((tp, share_rows, ff), BF16),
            pltpu.VMEM((n, tok_rows, width), BF16),
            pltpu.VMEM((tok_rows, width), F32),
            pltpu.VMEM((2, reach, tok_rows, width), BF16),
            dma((chips,)),
            dma((chips,)),
            dma((6,)),
            dma((6,)),
            dma((9,)),
            dma((9,)),
            dma((2, reach, REDUCE_PIECES)),
            dma((2, reach, REDUCE_PIECES)),
        ],
        compiler_params=pltpu.CompilerParams(collective_id=1, has_side_effects=True),
        cost_estimate=pl.CostEstimate(flops=2 * 10**9, bytes_accessed=10**7, transcendentals=0),
        name="expert_layer",
    )(rows, *weights, place)


def per_device(
    groups,
    n,
    tp,
    tokens,
    routes,
    routing_weight,
    norm_gain_vector,
    expert_gate,
    expert_up,
    expert_down,
    shared_gate,
    shared_up,
    shared_down,
):
    tok_rows, width = tokens.shape
    experts = expert_gate.shape[0]
    top_count = routes.shape[1]
    capacity = tok_rows * top_count * 7 // (6 * experts)
    gain = norm_gain_vector
    lanes = 128
    halves = []
    for whole in (
        (expert_gate * gain[None, None, :]).astype(BF16),
        (expert_up * gain[None, None, :]).astype(BF16),
        expert_down.astype(BF16),
    ):
        halves += [whole[:, :, c : c + lanes] for c in range(0, width, lanes)]
    share = -(-len(halves) // groups)
    first = lax.rem(lax.axis_index("grp") * share, len(halves))
    mine = lax.dynamic_slice_in_dim(
        jnp.stack(halves + halves[: share - 1], axis=1), first, share, axis=1
    )
    held = lax.all_to_all(mine, "fs", split_axis=0, concat_axis=0, tiled=True)

    values = tokens.astype(F32)
    totals = lax.psum(jnp.sum(values * values, axis=1), "tp")
    normed = (values * lax.rsqrt(totals / (width * tp) + norm_eps)[:, None]).astype(BF16)

    def as_lanes(a):
        return jnp.pad(a.T.astype(BF16), ((0, 0), (0, width - tok_rows)))

    block = jnp.concatenate(
        [
            normed,
            (shared_gate * gain[None, :]).astype(BF16),
            (shared_up * gain[None, :]).astype(BF16),
            shared_down.astype(BF16),
            as_lanes(routes),
            as_lanes(routing_weight),
        ],
        axis=0,
    )
    got, full = ring_gather(n, groups, len(halves), block, held)
    full = full.reshape(3, width // lanes, -1, lanes)
    gate_new, up_new, down_new = (
        jnp.concatenate([full[k, c] for c in range(width // lanes)], axis=1) for k in range(3)
    )
    unit = shared_gate.shape[0]
    at = tok_rows
    shared = []
    for _ in range(3):
        shared.append(got[:, at : at + unit, :].reshape(n * unit, width))
        at += unit
    sgate, sup, sdown = shared
    chosen_by = got[:, at : at + top_count, :tok_rows]
    weight_of = got[:, at + top_count : at + 2 * top_count, :tok_rows]
    mine = chosen_by.astype(F32) == lax.axis_index("fs").astype(F32)
    weights = jnp.sum(jnp.where(mine, weight_of.astype(F32), 0.0), axis=1)
    named = jnp.any(mine, axis=1)
    index = jnp.arange(tok_rows, dtype=jnp.int32)
    before = (index[:, None] < index[None, :]).astype(BF16)
    rank = jnp.dot(named.astype(BF16), before, preferred_element_type=F32)
    slot = jnp.where(named, rank, -1.0)
    hit = slot[:, None, :] == jnp.arange(capacity, dtype=jnp.int32).astype(F32)[None, :, None]
    place = jnp.where(hit, weights[:, None, :], 0.0).astype(BF16)
    picked = jnp.einsum(
        "bsj,bjd->bsd", hit.astype(BF16), got[:, :tok_rows, :], preferred_element_type=F32
    ).astype(BF16)
    per_share = n // tp * capacity
    shared_rows = tok_rows // tp
    rows = jnp.concatenate(
        [
            picked.reshape(tp, per_share, width),
            normed.reshape(tp, shared_rows, width),
            jnp.zeros((tp, -(per_share + shared_rows) % 32, width), BF16),
        ],
        axis=1,
    )
    mixed = run_layer(
        n,
        tp,
        tok_rows,
        rows,
        (gate_new, up_new, down_new, sgate, sup, sdown),
        place,
    )
    return (mixed, gate_new[None], up_new[None], down_new[None], sgate, sup, sdown)


def solution(mesh):
    return jax.shard_map(
        functools.partial(per_device, mesh.shape["grp"], mesh.shape["fs"], mesh.shape["tp"]),
        mesh=mesh,
        in_specs=(
            P(("grp", "fs"), "tp"),
            P(("grp", "fs"), None),
            P(("grp", "fs"), None),
            P("tp"),
            P(None, "fs", "tp"),
            P(None, "fs", "tp"),
            P(None, "fs", "tp"),
            P("fs", "tp"),
            P("fs", "tp"),
            P("fs", "tp"),
        ),
        out_specs=(
            P(("grp", "fs"), "tp"),
            P(("grp", "fs"), None, "tp"),
            P(("grp", "fs"), None, "tp"),
            P(("grp", "fs"), None, "tp"),
            P("grp", "tp"),
            P("grp", "tp"),
            P("grp", "tp"),
        ),
        check_vma=False,
    )
```
